32 devices in a mesh: sp: 16 (over z, y, core), tp: 2 (over x).
Axes of the slice: x: 2, y: 2, z: 4, core: 2. Of those that a mesh axis runs over, the one named last changes fastest.
Arguments:
- queries: bfloat16 [8192, 1024], P('sp', 'tp'), may hold values from -260 to 260, as said below
- keys: bfloat16 [8192, 512], P('sp', 'tp'), may hold values from -8 to 8, as said below
- values: bfloat16 [8192, 512], P('sp', 'tp'), may hold values from -24 to 24
- doc_ids: int32 [8192], P('sp'), may hold values from 0 to 3, never falling along the last dimension, each value on 1 to 4096 neighbouring positions
- sink_logit: float32 [8], P('tp'), may hold values from 2 to 7
- residual_in: bfloat16 [8192, 2048], P(('sp', 'tp')), may hold values from -6 to 6
- w_out: bfloat16 [1024, 2048], replicated, may hold values from -0.375 to 0.375
- gain_one: float32 [2048], replicated, may hold values from 0.1 to 1.9
- w_gate: bfloat16 [2048, 5632], P('sp', 'tp'), may hold values from -0.125 to 0.125
- w_up: bfloat16 [2048, 5632], P('sp', 'tp'), may hold values from -0.125 to 0.125
- w_down: bfloat16 [5632, 2048], P('tp', 'sp'), may hold values from -0.078125 to 0.078125
- gain_two: float32 [2048], replicated, may hold values from 0.1 to 1.9
Outputs:
- layer_out: bfloat16 [8192, 2048], P(('sp', 'tp'))
The draws below stay inside these ranges and needn't reach their ends.
Inputs may be any that keep to these rules, and one draw needn't show every extreme that they name: Real-valued projected queries. Real-valued projected keys. `doc_ids`: document numbers never fall along the sequence; each document is one run of positions.
All inputs are finite; a program needn't handle non-finite values.
Results may differ from the reference program's by a relative error of at most 0.012.
Values may be sent and summed in bfloat16 or wider, within the bound.
A program may use at most 128 MiB of HBM per device.

```python
import math
import jax
import jax.numpy as jnp
import numpy as np
from jax import lax

D = 2048
QH = 8
HEAD = 128
FF = 5632
HALF = 128
SEQ = 8192
QW = 1024
KVW = 512
FF_DEV = 2816
N_SP = 16
N_TP = 2


def paired_draw(key):
    key = jax.random.fold_in(key, 11)
    first_key, second_key = jax.random.split(key, 2)
    keys_f = jnp.clip(jax.random.normal(first_key, (SEQ, KVW), jnp.float32), -7.5, 7.5)
    queries_f = jnp.clip(jax.random.normal(second_key, (SEQ, QW), jnp.float32), -7.5, 7.5)
    return (queries_f, keys_f)


def draw_queries(key, part):
    return paired_draw(key)[0].astype(jnp.bfloat16)


def draw_keys(key, part):
    return paired_draw(key)[1].astype(jnp.bfloat16)


def levels(rng, shape, cuts, least, high):
    level = 1.0
    for axis_at, parts in cuts:
        steps = jax.random.uniform(jax.random.fold_in(jax.random.fold_in(rng, 6), axis_at), (parts,), jnp.float32, least / len(cuts), high / len(cuts))
        level = level * jnp.repeat(jnp.exp(steps), shape[axis_at] // parts).reshape((-1,) + (1,) * (len(shape) - 1 - axis_at))
    return level


def length_profile(count, total, most, skew):
    weights = [(1 << 20) // math.isqrt(standing ** skew) + 1 for standing in range(2, count + 1)]
    rest, counts = total - most - (count - 1), [1] * (count - 1)
    while rest > 0:
        candidates = [i for i in range(count - 1) if counts[i] < most]
        mass, budget = sum([weights[i] for i in candidates]), rest
        for i in candidates:
            more = min(most - counts[i], max(1, budget * weights[i] // mass), rest)
            counts[i] = counts[i] + more
            rest = rest - more
    return np.array([most] + counts)


def ragged_sizes(key, count, total, most, skew):
    if count == 2:
        one = jax.random.randint(key, (), max(1, total - most), min(most, total - 1) + 1)
        return jnp.stack([one, total - one])
    sizes = jnp.asarray(length_profile(count, total, most, skew), jnp.int32)
    twos = (count - 1) // 2
    donor, receiver = sizes[1:1 + 2 * twos:2], sizes[2:2 + 2 * twos:2]
    margin = jnp.minimum(donor - 1, most - receiver)
    moved = jax.random.randint(jax.random.fold_in(key, 1), (twos,), 0, 1 << 20) % (margin + 1)
    sizes = sizes.at[1:1 + 2 * twos:2].set(donor - moved).at[2:2 + 2 * twos:2].set(receiver + moved)
    return sizes[jax.random.permutation(jax.random.fold_in(key, 2), count)]


def scatter_about(stream_key, shape, spread, limit, cuts=(), kind=jnp.bfloat16):
    array = jax.random.normal(stream_key, shape, jnp.float32) * spread
    if len(cuts) > 0:
        array = levels(stream_key, shape, cuts, -0.22, 0.18) * array
    return jnp.clip(array, min=-limit, max=limit).astype(kind)


def setup_inputs(seed: int = 0) -> dict:
    key_list = jax.random.split(jax.random.key(seed), 13)
    return {
        "queries": draw_queries(jax.random.fold_in(key_list[12], 71), 0),
        "keys": draw_keys(jax.random.fold_in(key_list[12], 71), 0),
        "values": scatter_about(key_list[2], (SEQ, KVW), 4.0, 24.0, ((0, 16), (1, 2))),
        "doc_ids": jnp.searchsorted(jnp.cumsum(ragged_sizes(key_list[3], max(N_SP // 4, 2), SEQ, SEQ // 2, 1)), jnp.arange(SEQ), side="right").astype(jnp.int32),
        "sink_logit": jnp.clip(2.0 + 5.0 * jax.random.uniform(key_list[4], (QH,), jnp.float32) ** levels(key_list[4], (QH,), ((0, 2),), -0.2, 0.2), 2.0, 7.0),
        "residual_in": scatter_about(key_list[5], (SEQ, D), 1.0, 6.0, ((0, 32),)),
        "w_out": scatter_about(key_list[6], (QW, D), (QW // 4) ** -0.5, 0.375),
        "gain_one": jnp.clip(1.0 + 0.18 * jax.random.normal(key_list[7], (D,), jnp.float32), 0.1, 1.9),
        "w_gate": scatter_about(key_list[8], (D, FF), D ** -0.5, 0.125, ((0, 16), (1, 2))),
        "w_up": scatter_about(key_list[9], (D, FF), D ** -0.5, 0.125, ((0, 16), (1, 2))),
        "w_down": scatter_about(key_list[10], (FF, D), FF ** -0.5, 0.078125, ((0, 2), (1, 16))),
        "gain_two": jnp.clip(1.0 + 0.18 * jax.random.normal(key_list[11], (D,), jnp.float32), 0.1, 1.9),
    }


ALPHA = 2.0 ** 0.5
EPS = 1e-05
NEGATIVE = -1e+30

def layer_norm(values_in, gain):
    average = lax.optimization_barrier(jnp.mean(values_in, -1, keepdims=True))
    centred = values_in - average
    variance = lax.optimization_barrier(jnp.mean(centred * centred, -1, keepdims=True))
    return centred * lax.rsqrt(variance + EPS) * gain

def attend(queries, keys, values, doc_ids, sink_logit):
    seq_len = queries.shape[0]
    kv_heads = keys.shape[1] // HEAD
    repeat = queries.shape[1] // keys.shape[1]
    block = math.gcd(512, seq_len)
    span = block + 2 * HALF
    keys_pad = jnp.pad(keys, ((HALF, HALF), (0, 0)))
    values_pad = jnp.pad(values, ((HALF, HALF), (0, 0)))
    docs_pad = jnp.pad(doc_ids, (HALF, HALF), constant_values=-1)
    sinks = sink_logit.reshape(kv_heads, repeat)

    def one_block(index):
        start = index * block
        query_blk = lax.dynamic_slice_in_dim(queries, start, block, 0).reshape(block, kv_heads, repeat, HEAD)
        key_blk = lax.dynamic_slice_in_dim(keys_pad, start, span, 0).reshape(span, kv_heads, HEAD)
        value_blk = lax.dynamic_slice_in_dim(values_pad, start, span, 0).reshape(span, kv_heads, HEAD)
        doc_query = lax.dynamic_slice_in_dim(doc_ids, start, block, 0)
        doc_key = lax.dynamic_slice_in_dim(docs_pad, start, span, 0)
        pos_query = start + jnp.arange(block, dtype=jnp.int32)
        pos_key = start - HALF + jnp.arange(span, dtype=jnp.int32)
        offset = pos_key[None, :] - pos_query[:, None]
        allowed = (jnp.abs(offset) <= HALF) & (doc_key[None, :] == doc_query[:, None])
        allowed = allowed & (pos_key[None, :] >= 0) & (pos_key[None, :] < seq_len)
        scores = jnp.einsum('qgrd,kgd->grqk', query_blk.astype(jnp.float32), key_blk.astype(jnp.float32)) * HEAD ** (-0.5)
        scores = jnp.where(allowed[None, None], scores, NEGATIVE)
        top = jnp.maximum(lax.optimization_barrier(jnp.max(scores, -1)), sinks[:, :, None])
        weights = jnp.exp(scores - top[..., None])
        total = lax.optimization_barrier(jnp.sum(weights, -1)) + jnp.exp(sinks[:, :, None] - top)
        weights = weights.astype(jnp.bfloat16)
        summed = jnp.einsum('grqk,kgd->qgrd', weights.astype(jnp.float32), value_blk.astype(jnp.float32))
        scaled = summed / jnp.transpose(total, (2, 0, 1))[..., None]
        return scaled.reshape(block, kv_heads * repeat * HEAD).astype(jnp.bfloat16)
    blocks = lax.map(one_block, jnp.arange(seq_len // block, dtype=jnp.int32))
    return blocks.reshape(seq_len, -1)

def reference(queries, keys, values, doc_ids, sink_logit, residual_in, w_out, gain_one, w_gate, w_up, w_down, gain_two):
    attended = attend(queries, keys, values, doc_ids, sink_logit)
    mixed = jnp.dot(attended, w_out, preferred_element_type=jnp.float32)
    pre_one = ALPHA * residual_in.astype(jnp.float32) + mixed
    normed = layer_norm(pre_one, gain_one).astype(jnp.bfloat16)
    gate_part = jnp.dot(normed, w_gate, preferred_element_type=jnp.float32)
    up_part = jnp.dot(normed, w_up, preferred_element_type=jnp.float32)
    hidden = (jax.nn.silu(gate_part) * up_part).astype(jnp.bfloat16)

    def partial_down(carry, index):
        hidden_blk = lax.dynamic_slice_in_dim(hidden, index * FF_DEV, FF_DEV, 1)
        weight_blk = lax.dynamic_slice_in_dim(w_down, index * FF_DEV, FF_DEV, 0)
        term = jnp.dot(hidden_blk, weight_blk, preferred_element_type=jnp.float32).astype(jnp.bfloat16)
        term = lax.optimization_barrier(term).astype(jnp.float32)
        return (carry + term, None)
    down, _ = lax.scan(partial_down, jnp.zeros((SEQ, D), jnp.float32), jnp.arange(N_TP, dtype=jnp.int32))
    pre_two = ALPHA * normed.astype(jnp.float32) + down
    return layer_norm(pre_two, gain_two).astype(jnp.bfloat16)
```

```python
import functools
import math

import jax
import jax.numpy as jnp
from jax import lax
from jax.experimental import pallas as pl
from jax.experimental.pallas import tpu as pltpu
from jax.sharding import PartitionSpec as P

HEAD = 128
HALF = 128
CORES = 2
ALPHA = 2.0**0.5
EPS = 1e-05
NEGATIVE = -1e30
MESH = pl.DeviceIdType.MESH


def layer_norm(values_in, gain):
    average = jnp.mean(values_in, -1, keepdims=True)
    centred = values_in - average
    variance = jnp.mean(centred * centred, -1, keepdims=True)
    return centred * lax.rsqrt(variance + EPS) * gain


def kernel(
    sp_size,
    tp_size,
    q_ref,
    doc_col_ref,
    sink_ref,
    res_ref,
    gain_one_ref,
    gain_two_ref,
    k_hbm,
    v_hbm,
    doc_row_hbm,
    w_out_hbm,
    wg_hbm,
    wu_hbm,
    wd_hbm,
    out_ref,
    k_all,
    v_all,
    doc_all,
    w_out,
    gate_w,
    up_w,
    down_w,
    att,
    tokens,
    pre,
    normed,
    hidden,
    parts,
    others,
    local_sem,
    halo_send,
    halo_recv,
    ring_send,
    ring_recv,
    pair_send,
    pair_recv,
    tok_send,
    tok_recv,
    norm_send,
    norm_recv,
    sum_send,
    sum_recv,
):
    sp = lax.axis_index("sp")
    tp = lax.axis_index("tp")
    chips = sp_size // CORES
    y_size = math.gcd(tp_size, chips)
    z_size = chips // y_size
    half_ring = chips // 2
    core = lax.rem(sp, CORES)
    chip = sp // CORES
    my_y = lax.rem(chip, y_size)
    my_z = chip // y_size
    odd = lax.rem(my_y, 2)
    pos = my_y * z_size + my_z * (1 - odd) + (z_size - 1 - my_z) * odd

    def chip_at(steps):
        p = lax.rem(pos + (chips + steps), chips)
        y = p // z_size
        along = lax.rem(p, z_size)
        turned = lax.rem(y, 2)
        z = along * (1 - turned) + (z_size - 1 - along) * turned
        return z * y_size + y

    rows = q_ref.shape[0]
    token_rows = res_ref.shape[0]
    depth = wg_hbm.shape[0]
    cols_tp = q_ref.shape[1]
    kv_local = k_hbm.shape[1] // HEAD
    repeat = q_ref.shape[1] // k_hbm.shape[1]
    width = res_ref.shape[1]

    forward = (chip_at(1) * CORES + core, tp)
    backward = (chip_at(-1) * CORES + core, tp)
    partner = (chip * CORES + (1 - core), tp)
    after = (lax.rem(sp + 1, sp_size), tp)
    before = (lax.rem(sp + sp_size - 1, sp_size), tp)
    peers = [lax.rem(tp + i, tp_size) for i in range(1, tp_size)]

    barrier = pltpu.get_barrier_semaphore()
    greeted = [forward, backward, partner, after, before] + [(sp, j) for j in peers]
    for device in greeted:
        pl.semaphore_signal(barrier, inc=1, device_id=device, device_id_type=MESH)

    loads = [
        pltpu.make_async_copy(k_hbm, k_all.at[pl.ds(HALF, rows)], local_sem.at[0]),
        pltpu.make_async_copy(v_hbm, v_all.at[pl.ds(HALF, rows)], local_sem.at[1]),
        pltpu.make_async_copy(doc_row_hbm, doc_all.at[:, pl.ds(HALF, rows)], local_sem.at[2]),
        pltpu.make_async_copy(w_out_hbm, w_out, local_sem.at[3]),
    ]
    mine = pl.multiple_of(sp * depth, depth)
    own_loads = [
        pltpu.make_async_copy(src, dst.at[pl.ds(mine, depth)], local_sem.at[4 + i])
        for i, (src, dst) in enumerate(((wg_hbm, gate_w), (wu_hbm, up_w), (wd_hbm, down_w)))
    ]
    for load in loads + own_loads:
        load.start()
    pl.semaphore_wait(barrier, len(greeted))

    def remote(src, dst, send, recv, device):
        return pltpu.make_async_remote_copy(
            src_ref=src, dst_ref=dst, send_sem=send, recv_sem=recv, device_id=device, device_id_type=MESH
        )

    low, high = (pl.ds(0, HALF), pl.ds(rows - HALF, HALF))
    into_low, into_high = (pl.ds(0, HALF), pl.ds(HALF + rows, HALF))
    halos = []
    for i, (src, dst) in enumerate(((k_hbm, k_all), (v_hbm, v_all))):
        halos.append(
            remote(src.at[high], dst.at[into_low], halo_send.at[i, 0], halo_recv.at[i, 0], after)
        )
        halos.append(
            remote(src.at[low], dst.at[into_high], halo_send.at[i, 1], halo_recv.at[i, 1], before)
        )
    halos.append(
        remote(
            doc_row_hbm.at[:, high], doc_all.at[:, into_low], halo_send.at[2, 0], halo_recv.at[2, 0], after
        )
    )
    halos.append(
        remote(
            doc_row_hbm.at[:, low], doc_all.at[:, into_high], halo_send.at[2, 1], halo_recv.at[2, 1], before
        )
    )
    for halo in halos:
        halo.start()

    part_rows = depth // 2
    pieces = (
        (wg_hbm, gate_w, 0, depth),
        (wu_hbm, up_w, 0, depth),
        (wd_hbm, down_w, 0, part_rows),
        (wd_hbm, down_w, part_rows, part_rows),
    )

    def place(piece, chip_id, core_id):
        _, buf, first, count = pieces[piece]
        start = pl.multiple_of((chip_id * CORES + core_id) * depth + first, count)
        return buf.at[pl.ds(start, count)]

    def own(piece):
        src, _, first, count = pieces[piece]
        return src.at[pl.ds(first, count)]

    def ring_out(way, piece, distance):
        steps = -(distance - 1) if way == 0 else distance - 1
        dst = place(piece, chip_at(steps), core)
        src = own(piece) if distance == 1 else dst
        return remote(
            src,
            dst,
            ring_send.at[way, piece, distance],
            ring_recv.at[way, piece, distance],
            forward if way == 0 else backward,
        )

    def ring_in(way, piece, distance):
        dst = place(piece, chip_at(-distance if way == 0 else distance), core)
        return remote(
            dst,
            dst,
            ring_send.at[way, piece, distance],
            ring_recv.at[way, piece, distance],
            backward if way == 0 else forward,
        )

    def pair(way, piece, distance, core_id):
        steps = 0 if distance == 0 else (-distance if way == 0 else distance)
        dst = place(piece, chip_at(steps), core_id)
        src = own(piece) if distance == 0 else dst
        return remote(
            src, dst, pair_send.at[way, piece, distance], pair_recv.at[way, piece, distance], partner
        )

    def pair_in(way, piece, distance):
        steps = 0 if distance == 0 else (-distance if way == 0 else distance)
        dst = place(piece, chip_at(steps), 1 - core)
        return remote(
            dst, dst, pair_send.at[way, piece, distance], pair_recv.at[way, piece, distance], partner
        )

    sent = []

    def launch(copy):
        copy.start()
        sent.append(copy)

    rounds = []
    for both in ((0, 1), (2, 3)):
        for distance in range(1, half_ring + 1):
            rounds.append((distance, both[0], both[1]))
            if distance < half_ring:
                rounds.append((distance, both[1], both[0]))
    legs = [set(), set()]
    for distance, first, second in rounds:
        legs[0].add((distance, first))
        legs[1].add((distance, second))
    per_phase = len(rounds) // 2

    def pump(index):
        distance, first, second = rounds[index]
        for way, piece in ((0, first), (1, second)):
            ring_in(way, piece, distance).wait_recv()
            if (distance + 1, piece) in legs[way]:
                launch(ring_out(way, piece, distance + 1))
            launch(pair(way, piece, distance, core))
        if index == per_phase - 2:
            launch(ring_out(0, 2, 1))
            launch(ring_out(1, 3, 1))
        if index == per_phase - 1:
            launch(ring_out(0, 3, 1))
            launch(ring_out(1, 2, 1))

    launch(ring_out(0, 0, 1))
    launch(ring_out(1, 1, 1))
    launch(ring_out(0, 1, 1))
    launch(ring_out(1, 0, 1))
    for piece in range(4):
        launch(pair(0, piece, 0, core))

    for load in loads[:3]:
        load.wait()
    for halo in halos:
        halo.wait_recv()
    span = rows + 2 * HALF
    at = lax.broadcasted_iota(jnp.int32, (1, span), 1) + (sp * rows - HALF)
    inside = jnp.logical_and(at >= 0, at < sp_size * rows)
    doc_keys = jnp.where(inside, doc_all[...], -1)
    reach = 3 * HALF
    offset = lax.broadcasted_iota(jnp.int32, (HALF, reach), 1) - lax.broadcasted_iota(
        jnp.int32, (HALF, reach), 0
    )
    near = jnp.logical_and(offset >= 0, offset <= 2 * HALF)
    for block in range(rows // HALF):
        doc_query = doc_col_ref[block * HALF : (block + 1) * HALF, :]
        same = doc_query == doc_keys[:, block * HALF : block * HALF + reach]
        allowed = jnp.logical_and(near, same)
        for group in range(kv_local):
            lanes = slice(group * HEAD, (group + 1) * HEAD)
            key_blk = k_all[block * HALF : block * HALF + reach, lanes]
            value_blk = v_all[block * HALF : block * HALF + reach, lanes]
            for r in range(repeat):
                h = group * repeat + r
                query_blk = q_ref[block * HALF : (block + 1) * HALF, h * HEAD : (h + 1) * HEAD]
                scores = lax.dot_general(
                    query_blk, key_blk, (((1,), (1,)), ((), ())), preferred_element_type=jnp.float32
                ) * HEAD ** (-0.5)
                scores = jnp.where(allowed, scores, NEGATIVE)
                sink = sink_ref[h : h + 1, 0:1]
                top = jnp.maximum(jnp.max(scores, -1, keepdims=True), sink)
                weights = jnp.exp(scores - top)
                total = jnp.sum(weights, -1, keepdims=True) + jnp.exp(sink - top)
                summed = jnp.dot(
                    weights.astype(jnp.bfloat16), value_blk, preferred_element_type=jnp.float32
                )
                att[block * HALF : (block + 1) * HALF, h * HEAD : (h + 1) * HEAD] = (
                    summed / total
                ).astype(jnp.bfloat16)

    my_rows = pl.ds(pl.multiple_of(tp * token_rows, token_rows), token_rows)
    tokens[pl.ds(tp, 1)] = att[my_rows, :][None]
    pump(0)
    for i, j in enumerate(peers):
        launch(
            remote(
                att.at[pl.ds(pl.multiple_of(j * token_rows, token_rows), token_rows)],
                tokens.at[tp],
                tok_send.at[i],
                tok_recv.at[i],
                (sp, j),
            )
        )
    loads[3].wait()
    for i in range(tp_size - 1):
        source = lax.rem(tp + (tp_size - 1 - i), tp_size)
        slot = tokens.at[source]
        remote(slot, slot, tok_send.at[i], tok_recv.at[i], (sp, source)).wait_recv()
    tile = min(512, width)

    @pl.loop(0, width // tile)
    def _(t):
        lanes = pl.ds(pl.multiple_of(t * tile, tile), tile)
        mixed = ALPHA * res_ref[:, lanes].astype(jnp.float32)
        for j in range(tp_size):
            mixed += jnp.dot(
                tokens[j],
                w_out[j * cols_tp : (j + 1) * cols_tp, lanes],
                preferred_element_type=jnp.float32,
            )
        pre[:, lanes] = mixed

    strip = math.gcd(32, token_rows)

    @pl.loop(0, token_rows // strip)
    def _(t):
        here = pl.ds(pl.multiple_of(t * strip, strip), strip)
        there = pl.ds(pl.multiple_of(tp * token_rows + t * strip, strip), strip)
        normed[there, :] = layer_norm(pre[here, :], gain_one_ref[...]).astype(jnp.bfloat16)

    pump(1)
    for i, j in enumerate(peers):
        launch(
            remote(
                normed.at[my_rows], normed.at[my_rows], norm_send.at[i], norm_recv.at[i], (sp, j)
            )
        )
    for index in range(2, per_phase):
        pump(index)

    for load in own_loads:
        load.wait()
    for piece in (0, 1):
        pair_in(0, piece, 0).wait_recv()
    for distance, first, second in rounds[:per_phase]:
        pair_in(0, first, distance).wait_recv()
        pair_in(1, second, distance).wait_recv()
    for i in range(tp_size - 1):
        source = lax.rem(tp + (tp_size - 1 - i), tp_size)
        slot = normed.at[pl.ds(pl.multiple_of(source * token_rows, token_rows), token_rows)]
        remote(slot, slot, norm_send.at[i], norm_recv.at[i], (sp, source)).wait_recv()

    units = wg_hbm.shape[1]
    block_units = 256 if units % 256 == 0 else 128
    steps = units // block_units

    def hidden_tiles(first, last):
        @pl.loop(first, last)
        def _(t):
            lanes = pl.ds(pl.multiple_of(t * block_units, block_units), block_units)
            gate = jnp.dot(normed[...], gate_w[:, lanes], preferred_element_type=jnp.float32)
            up = jnp.dot(normed[...], up_w[:, lanes], preferred_element_type=jnp.float32)
            hidden[:, lanes] = (gate / (1.0 + jnp.exp(-gate)) * up).astype(jnp.bfloat16)

    middle = steps // 2
    hidden_tiles(0, middle)
    pump(per_phase)
    hidden_tiles(middle, steps)
    pump(per_phase + 1)

    chunk = CORES * depth
    order = []

    def chunk_sends(number, owner):
        lanes = pl.ds(pl.multiple_of(owner * chunk, chunk), chunk)
        for i, j in enumerate(peers):
            launch(
                remote(
                    parts.at[j, :, lanes],
                    others.at[i, :, lanes],
                    sum_send.at[number, i],
                    sum_recv.at[number, i],
                    (sp, j),
                )
            )

    def down_chunk(owner):
        start = pl.multiple_of(owner * chunk, chunk)
        part = lax.dot_general(
            hidden[...],
            down_w[pl.ds(start, chunk), :],
            (((1,), (1,)), ((), ())),
            preferred_element_type=jnp.float32,
        ).astype(jnp.bfloat16)
        for j in range(tp_size):
            parts[j, :, pl.ds(start, chunk)] = part[j * token_rows : (j + 1) * token_rows, :]
        order.append(owner)
        if len(order) > 1:
            chunk_sends(len(order) - 2, order[-2])

    for piece in (2, 3):
        pair_in(0, piece, 0).wait_recv()
    down_chunk(chip_at(0))
    index = per_phase + 2
    for distance in range(1, half_ring + 1):
        if distance == half_ring:
            pump(index)
            index += 1
            pair_in(0, 2, distance).wait_recv()
            pair_in(1, 3, distance).wait_recv()
            down_chunk(chip_at(distance))
            continue
        if distance > 1:
            pump(index)
            pump(index + 1)
            index += 2
        for piece in (2, 3):
            pair_in(0, piece, distance).wait_recv()
            pair_in(1, piece, distance).wait_recv()
        down_chunk(chip_at(-distance))
        down_chunk(chip_at(distance))
    chunk_sends(len(order) - 1, order[-1])
    for number, owner in enumerate(order):
        lanes = pl.ds(pl.multiple_of(owner * chunk, chunk), chunk)
        for i in range(tp_size - 1):
            source = lax.rem(tp + (tp_size - 1 - i), tp_size)
            slot = others.at[i, :, lanes]
            remote(slot, slot, sum_send.at[number, i], sum_recv.at[number, i], (sp, source)).wait_recv()

    @pl.loop(0, token_rows // strip)
    def _(t):
        here = pl.ds(pl.multiple_of(t * strip, strip), strip)
        there = pl.ds(pl.multiple_of(tp * token_rows + t * strip, strip), strip)
        down = parts[pl.ds(tp, 1), here, :][0].astype(jnp.float32)
        for i in range(tp_size - 1):
            down += others[i, here, :].astype(jnp.float32)
        pre_two = ALPHA * normed[there, :].astype(jnp.float32) + down
        out_ref[here, :] = layer_norm(pre_two, gain_two_ref[...]).astype(jnp.bfloat16)

    for halo in halos:
        halo.wait_send()
    for copy in sent:
        copy.wait_send()


def solution(mesh):
    sp_size = mesh.shape["sp"]
    tp_size = mesh.shape["tp"]

    def per_device(
        queries,
        keys,
        values,
        doc_ids,
        sink_logit,
        residual_in,
        w_out,
        gain_one,
        w_gate,
        w_up,
        w_down,
        gain_two,
    ):
        rows = queries.shape[0]
        token_rows, width = residual_in.shape
        units = w_gate.shape[1]
        span = rows + 2 * HALF
        chips = sp_size // CORES
        full = w_gate.shape[0] * sp_size
        bf16, f32 = (jnp.bfloat16, jnp.float32)
        dma = pltpu.SemaphoreType.DMA
        others = max(tp_size - 1, 1)
        vmem, anywhere = (pl.BlockSpec(memory_space=pltpu.VMEM), pl.BlockSpec(memory_space=pl.ANY))
        return pl.pallas_call(
            functools.partial(kernel, sp_size, tp_size),
            out_shape=jax.ShapeDtypeStruct((token_rows, width), bf16),
            in_specs=[vmem] * 6 + [anywhere] * 7,
            out_specs=vmem,
            scratch_shapes=[
                pltpu.VMEM((span, keys.shape[1]), bf16),
                pltpu.VMEM((span, keys.shape[1]), bf16),
                pltpu.VMEM((1, span), jnp.int32),
                pltpu.VMEM(w_out.shape, bf16),
                pltpu.VMEM((full, units), bf16),
                pltpu.VMEM((full, units), bf16),
                pltpu.VMEM((w_down.shape[1] * sp_size, units), bf16),
                pltpu.VMEM((rows, queries.shape[1]), bf16),
                pltpu.VMEM((tp_size, token_rows, queries.shape[1]), bf16),
                pltpu.VMEM((token_rows, width), f32),
                pltpu.VMEM((rows, width), bf16),
                pltpu.VMEM((rows, units), bf16),
                pltpu.VMEM((tp_size, token_rows, width), bf16),
                pltpu.VMEM((others, token_rows, width), bf16),
                dma((7,)),
                dma((3, 2)),
                dma((3, 2)),
                dma((2, 4, chips // 2 + 1)),
                dma((2, 4, chips // 2 + 1)),
                dma((2, 4, chips // 2 + 1)),
                dma((2, 4, chips // 2 + 1)),
                dma((others,)),
                dma((others,)),
                dma((others,)),
                dma((others,)),
                dma((chips, others)),
                dma((chips, others)),
            ],
            compiler_params=pltpu.CompilerParams(
                collective_id=0, has_side_effects=True, vmem_limit_bytes=62 * 2**20
            ),
        )(
            queries,
            doc_ids[:, None],
            jnp.broadcast_to(sink_logit[:, None], (sink_logit.shape[0], HEAD)),
            residual_in,
            gain_one[None, :],
            gain_two[None, :],
            keys,
            values,
            doc_ids[None, :],
            w_out,
            w_gate,
            w_up,
            w_down.T,
        )

    in_specs = (
        P("sp", "tp"),
        P("sp", "tp"),
        P("sp", "tp"),
        P("sp"),
        P("tp"),
        P(("sp", "tp"), None),
        P(),
        P(),
        P("sp", "tp"),
        P("sp", "tp"),
        P("tp", "sp"),
        P(),
    )
    return jax.shard_map(
        per_device, mesh=mesh, in_specs=in_specs, out_specs=P(("sp", "tp"), None), check_vma=False
    )
```

```python
import functools
import math

import jax
import jax.numpy as jnp
from jax import lax
from jax.experimental import pallas as pl
from jax.experimental.pallas import tpu as pltpu
from jax.sharding import PartitionSpec as P

HEAD = 128
HALF = 128
CORES = 2
ALPHA = 2.0**0.5
EPS = 1e-05
NEGATIVE = -1e30
MESH = pl.DeviceIdType.MESH


def layer_norm(values_in, gain):
    average = jnp.mean(values_in, -1, keepdims=True)
    centred = values_in - average
    variance = jnp.mean(centred * centred, -1, keepdims=True)
    return centred * lax.rsqrt(variance + EPS) * gain


def kernel(
    sp_size,
    tp_size,
    q_ref,
    sink_ref,
    res_ref,
    gain_one_ref,
    gain_two_ref,
    k_hbm,
    v_hbm,
    doc_row_hbm,
    w_out_hbm,
    wg_hbm,
    wu_hbm,
    wd_hbm,
    out_ref,
    k_all,
    v_all,
    doc_all,
    w_out,
    gate_w,
    up_w,
    down_w,
    att,
    tokens,
    pre,
    normed,
    hidden,
    down_in,
    parts,
    others,
    local_sem,
    halo_send,
    halo_recv,
    ring_send,
    ring_recv,
    pair_send,
    pair_recv,
    tok_send,
    tok_recv,
    norm_send,
    norm_recv,
    sum_send,
    sum_recv,
):
    sp = lax.axis_index("sp")
    tp = lax.axis_index("tp")
    chips = sp_size // CORES
    y_size = math.gcd(tp_size, chips)
    z_size = chips // y_size
    half_ring = chips // 2
    core = lax.rem(sp, CORES)
    chip = sp // CORES
    my_y = lax.rem(chip, y_size)
    my_z = chip // y_size
    odd = lax.rem(my_y, 2)
    pos = my_y * z_size + my_z * (1 - odd) + (z_size - 1 - my_z) * odd

    def chip_at(steps):
        p = lax.rem(pos + (chips + steps), chips)
        y = p // z_size
        along = lax.rem(p, z_size)
        turned = lax.rem(y, 2)
        z = along * (1 - turned) + (z_size - 1 - along) * turned
        return z * y_size + y

    rows = q_ref.shape[0]
    token_rows = res_ref.shape[0]
    depth = wg_hbm.shape[0]
    cols_tp = q_ref.shape[1]
    kv_local = k_hbm.shape[1] // HEAD
    repeat = q_ref.shape[1] // k_hbm.shape[1]
    width = res_ref.shape[1]

    forward = (chip_at(1) * CORES + core, tp)
    backward = (chip_at(-1) * CORES + core, tp)
    partner = (chip * CORES + (1 - core), tp)
    after = (lax.rem(sp + 1, sp_size), tp)
    before = (lax.rem(sp + sp_size - 1, sp_size), tp)
    peers = [lax.rem(tp + i, tp_size) for i in range(1, tp_size)]

    barrier = pltpu.get_barrier_semaphore()
    greeted = [forward, backward, partner, after, before] + [(sp, j) for j in peers]
    for device in greeted:
        pl.semaphore_signal(barrier, inc=1, device_id=device, device_id_type=MESH)

    loads = [
        pltpu.make_async_copy(k_hbm, k_all.at[pl.ds(HALF, rows)], local_sem.at[0]),
        pltpu.make_async_copy(v_hbm, v_all.at[pl.ds(HALF, rows)], local_sem.at[1]),
        pltpu.make_async_copy(doc_row_hbm, doc_all.at[:, pl.ds(HALF, rows)], local_sem.at[2]),
        pltpu.make_async_copy(w_out_hbm, w_out, local_sem.at[3]),
    ]
    mine = pl.multiple_of(sp * depth, depth)
    own_loads = [
        pltpu.make_async_copy(src, dst.at[pl.ds(mine, depth)], local_sem.at[4 + i])
        for i, (src, dst) in enumerate(((wg_hbm, gate_w), (wu_hbm, up_w)))
    ]
    down_load = pltpu.make_async_copy(wd_hbm, down_in, local_sem.at[6])
    for load in loads + own_loads + [down_load]:
        load.start()
    pl.semaphore_wait(barrier, len(greeted))

    def remote(src, dst, send, recv, device):
        return pltpu.make_async_remote_copy(
            src_ref=src, dst_ref=dst, send_sem=send, recv_sem=recv, device_id=device, device_id_type=MESH
        )

    low, high = (pl.ds(0, HALF), pl.ds(rows - HALF, HALF))
    into_low, into_high = (pl.ds(0, HALF), pl.ds(HALF + rows, HALF))
    halos = []
    for i, (src, dst) in enumerate(((k_hbm, k_all), (v_hbm, v_all))):
        halos.append(
            remote(src.at[high], dst.at[into_low], halo_send.at[i, 0], halo_recv.at[i, 0], after)
        )
        halos.append(
            remote(src.at[low], dst.at[into_high], halo_send.at[i, 1], halo_recv.at[i, 1], before)
        )
    halos.append(
        remote(
            doc_row_hbm.at[:, high], doc_all.at[:, into_low], halo_send.at[2, 0], halo_recv.at[2, 0], after
        )
    )
    halos.append(
        remote(
            doc_row_hbm.at[:, low], doc_all.at[:, into_high], halo_send.at[2, 1], halo_recv.at[2, 1], before
        )
    )
    for halo in halos:
        halo.start()

    part_rows = depth // 2
    pieces = (
        (wg_hbm, gate_w, 0, depth),
        (wu_hbm, up_w, 0, depth),
        (None, down_w, 0, part_rows),
        (None, down_w, part_rows, part_rows),
    )

    def place(piece, chip_id, core_id):
        _, buf, first, count = pieces[piece]
        start = pl.multiple_of((chip_id * CORES + core_id) * depth + first, count)
        return buf.at[pl.ds(start, count)]

    def own(piece):
        src, _, first, count = pieces[piece]
        if src is None:
            return place(piece, chip, core)
        return src.at[pl.ds(first, count)]

    def ring_out(way, piece, distance):
        steps = -(distance - 1) if way == 0 else distance - 1
        dst = place(piece, chip_at(steps), core)
        src = own(piece) if distance == 1 else dst
        return remote(
            src,
            dst,
            ring_send.at[way, piece, distance],
            ring_recv.at[way, piece, distance],
            forward if way == 0 else backward,
        )

    def ring_in(way, piece, distance):
        dst = place(piece, chip_at(-distance if way == 0 else distance), core)
        return remote(
            dst,
            dst,
            ring_send.at[way, piece, distance],
            ring_recv.at[way, piece, distance],
            backward if way == 0 else forward,
        )

    def pair(way, piece, distance, core_id):
        steps = 0 if distance == 0 else (-distance if way == 0 else distance)
        dst = place(piece, chip_at(steps), core_id)
        src = own(piece) if distance == 0 else dst
        return remote(
            src, dst, pair_send.at[way, piece, distance], pair_recv.at[way, piece, distance], partner
        )

    def pair_in(way, piece, distance):
        steps = 0 if distance == 0 else (-distance if way == 0 else distance)
        dst = place(piece, chip_at(steps), 1 - core)
        return remote(
            dst, dst, pair_send.at[way, piece, distance], pair_recv.at[way, piece, distance], partner
        )

    sent = []

    def launch(copy):
        copy.start()
        sent.append(copy)

    rounds = []
    for both in ((0, 1), (2, 3)):
        for distance in range(1, half_ring + 1):
            rounds.append((distance, both[0], both[1]))
            if distance < half_ring:
                rounds.append((distance, both[1], both[0]))
    legs = [set(), set()]
    for distance, first, second in rounds:
        legs[0].add((distance, first))
        legs[1].add((distance, second))
    per_phase = len(rounds) // 2

    def pump(index):
        distance, first, second = rounds[index]
        for way, piece in ((0, first), (1, second)):
            ring_in(way, piece, distance).wait_recv()
            if (distance + 1, piece) in legs[way]:
                launch(ring_out(way, piece, distance + 1))
            launch(pair(way, piece, distance, core))
        if index == per_phase - 2:
            launch(ring_out(0, 2, 1))
            launch(ring_out(1, 3, 1))
        if index == per_phase - 1:
            launch(ring_out(0, 3, 1))
            launch(ring_out(1, 2, 1))

    launch(ring_out(0, 0, 1))
    launch(ring_out(1, 1, 1))
    launch(ring_out(0, 1, 1))
    launch(ring_out(1, 0, 1))
    for piece in (0, 1):
        launch(pair(0, piece, 0, core))
    down_load.wait()
    down_w[pl.ds(mine, depth), :] = down_in[...].T

    for load in loads[:3]:
        load.wait()
    for halo in halos:
        halo.wait_recv()
    span = rows + 2 * HALF
    at = lax.broadcasted_iota(jnp.int32, (1, span), 1) + (sp * rows - HALF)
    inside = jnp.logical_and(at >= 0, at < sp_size * rows)
    doc_keys = jnp.where(inside, doc_all[...], -1)
    reach = 3 * HALF
    offset = lax.broadcasted_iota(jnp.int32, (HALF, reach), 1) - lax.broadcasted_iota(
        jnp.int32, (HALF, reach), 0
    )
    near = jnp.logical_and(offset >= 0, offset <= 2 * HALF)
    for block in range(rows // HALF):
        doc_row = doc_all[:, (block + 1) * HALF : (block + 2) * HALF]
        doc_query = jnp.broadcast_to(doc_row, (HALF, HALF)).T
        same = jnp.concatenate([doc_query] * 3, 1) == doc_keys[:, block * HALF : block * HALF + reach]
        allowed = jnp.logical_and(near, same)
        for group in range(kv_local):
            lanes = slice(group * HEAD, (group + 1) * HEAD)
            key_blk = k_all[block * HALF : block * HALF + reach, lanes]
            value_blk = v_all[block * HALF : block * HALF + reach, lanes]
            for r in range(repeat):
                h = group * repeat + r
                query_blk = q_ref[block * HALF : (block + 1) * HALF, h * HEAD : (h + 1) * HEAD]
                scores = lax.dot_general(
                    query_blk, key_blk, (((1,), (1,)), ((), ())), preferred_element_type=jnp.float32
                ) * HEAD ** (-0.5)
                scores = jnp.where(allowed, scores, NEGATIVE)
                sink = jnp.full((1, 1), sink_ref[h], jnp.float32)
                top = jnp.maximum(jnp.max(scores, -1, keepdims=True), sink)
                weights = jnp.exp(scores - top)
                total = jnp.sum(weights, -1, keepdims=True) + jnp.exp(sink - top)
                summed = jnp.dot(
                    weights.astype(jnp.bfloat16), value_blk, preferred_element_type=jnp.float32
                )
                att[block * HALF : (block + 1) * HALF, h * HEAD : (h + 1) * HEAD] = (
                    summed / total
                ).astype(jnp.bfloat16)

    for piece in (2, 3):
        launch(pair(0, piece, 0, core))

    my_rows = pl.ds(pl.multiple_of(tp * token_rows, token_rows), token_rows)
    tokens[pl.ds(tp, 1)] = att[my_rows, :][None]
    pump(0)
    for i, j in enumerate(peers):
        launch(
            remote(
                att.at[pl.ds(pl.multiple_of(j * token_rows, token_rows), token_rows)],
                tokens.at[tp],
                tok_send.at[i],
                tok_recv.at[i],
                (sp, j),
            )
        )
    loads[3].wait()
    for i in range(tp_size - 1):
        source = lax.rem(tp + (tp_size - 1 - i), tp_size)
        slot = tokens.at[source]
        remote(slot, slot, tok_send.at[i], tok_recv.at[i], (sp, source)).wait_recv()
    tile = min(512, width)

    @pl.loop(0, width // tile)
    def _(t):
        lanes = pl.ds(pl.multiple_of(t * tile, tile), tile)
        mixed = ALPHA * res_ref[:, lanes].astype(jnp.float32)
        for j in range(tp_size):
            mixed += jnp.dot(
                tokens[j],
                w_out[j * cols_tp : (j + 1) * cols_tp, lanes],
                preferred_element_type=jnp.float32,
            )
        pre[:, lanes] = mixed

    strip = math.gcd(32, token_rows)

    @pl.loop(0, token_rows // strip)
    def _(t):
        here = pl.ds(pl.multiple_of(t * strip, strip), strip)
        there = pl.ds(pl.multiple_of(tp * token_rows + t * strip, strip), strip)
        normed[there, :] = layer_norm(pre[here, :], gain_one_ref[...]).astype(jnp.bfloat16)

    pump(1)
    for i, j in enumerate(peers):
        launch(
            remote(
                normed.at[my_rows], normed.at[my_rows], norm_send.at[i], norm_recv.at[i], (sp, j)
            )
        )
    for index in range(2, per_phase):
        pump(index)

    for load in own_loads:
        load.wait()
    for piece in (0, 1):
        pair_in(0, piece, 0).wait_recv()
    for distance, first, second in rounds[:per_phase]:
        pair_in(0, first, distance).wait_recv()
        pair_in(1, second, distance).wait_recv()
    for i in range(tp_size - 1):
        source = lax.rem(tp + (tp_size - 1 - i), tp_size)
        slot = normed.at[pl.ds(pl.multiple_of(source * token_rows, token_rows), token_rows)]
        remote(slot, slot, norm_send.at[i], norm_recv.at[i], (sp, source)).wait_recv()

    units = wg_hbm.shape[1]
    block_units = 256 if units % 256 == 0 else 128
    steps = units // block_units

    def hidden_tiles(first, last):
        @pl.loop(first, last)
        def _(t):
            lanes = pl.ds(pl.multiple_of(t * block_units, block_units), block_units)
            gate = jnp.dot(normed[...], gate_w[:, lanes], preferred_element_type=jnp.float32)
            up = jnp.dot(normed[...], up_w[:, lanes], preferred_element_type=jnp.float32)
            hidden[:, lanes] = (gate / (1.0 + jnp.exp(-gate)) * up).astype(jnp.bfloat16)

    middle = steps // 2
    hidden_tiles(0, middle)
    pump(per_phase)
    hidden_tiles(middle, steps)
    pump(per_phase + 1)

    chunk = CORES * depth
    order = []

    def chunk_sends(number, owner):
        lanes = pl.ds(pl.multiple_of(owner * chunk, chunk), chunk)
        for i, j in enumerate(peers):
            launch(
                remote(
                    parts.at[j, :, lanes],
                    others.at[i, :, lanes],
                    sum_send.at[number, i],
                    sum_recv.at[number, i],
                    (sp, j),
                )
            )

    def down_chunk(owner):
        start = pl.multiple_of(owner * chunk, chunk)
        part = lax.dot_general(
            hidden[...],
            down_w[pl.ds(start, chunk), :],
            (((1,), (1,)), ((), ())),
            preferred_element_type=jnp.float32,
        ).astype(jnp.bfloat16)
        for j in range(tp_size):
            parts[j, :, pl.ds(start, chunk)] = part[j * token_rows : (j + 1) * token_rows, :]
        order.append(owner)
        if len(order) > 1:
            chunk_sends(len(order) - 2, order[-2])

    for piece in (2, 3):
        pair_in(0, piece, 0).wait_recv()
    down_chunk(chip_at(0))
    index = per_phase + 2
    for distance in range(1, half_ring + 1):
        if distance == half_ring:
            pump(index)
            index += 1
            pair_in(0, 2, distance).wait_recv()
            pair_in(1, 3, distance).wait_recv()
            down_chunk(chip_at(distance))
            continue
        if distance > 1:
            pump(index)
            pump(index + 1)
            index += 2
        for piece in (2, 3):
            pair_in(0, piece, distance).wait_recv()
            pair_in(1, piece, distance).wait_recv()
        down_chunk(chip_at(-distance))
        down_chunk(chip_at(distance))
    chunk_sends(len(order) - 1, order[-1])
    for number, owner in enumerate(order):
        lanes = pl.ds(pl.multiple_of(owner * chunk, chunk), chunk)
        for i in range(tp_size - 1):
            source = lax.rem(tp + (tp_size - 1 - i), tp_size)
            slot = others.at[i, :, lanes]
            remote(slot, slot, sum_send.at[number, i], sum_recv.at[number, i], (sp, source)).wait_recv()

    @pl.loop(0, token_rows // strip)
    def _(t):
        here = pl.ds(pl.multiple_of(t * strip, strip), strip)
        there = pl.ds(pl.multiple_of(tp * token_rows + t * strip, strip), strip)
        down = parts[pl.ds(tp, 1), here, :][0].astype(jnp.float32)
        for i in range(tp_size - 1):
            down += others[i, here, :].astype(jnp.float32)
        pre_two = ALPHA * normed[there, :].astype(jnp.float32) + down
        out_ref[here, :] = layer_norm(pre_two, gain_two_ref[...]).astype(jnp.bfloat16)

    for halo in halos:
        halo.wait_send()
    for copy in sent:
        copy.wait_send()


def solution(mesh):
    sp_size = mesh.shape["sp"]
    tp_size = mesh.shape["tp"]

    def per_device(
        queries,
        keys,
        values,
        doc_ids,
        sink_logit,
        residual_in,
        w_out,
        gain_one,
        w_gate,
        w_up,
        w_down,
        gain_two,
    ):
        rows = queries.shape[0]
        token_rows, width = residual_in.shape
        units = w_gate.shape[1]
        span = rows + 2 * HALF
        chips = sp_size // CORES
        full = w_gate.shape[0] * sp_size
        bf16, f32 = (jnp.bfloat16, jnp.float32)
        dma = pltpu.SemaphoreType.DMA
        others = max(tp_size - 1, 1)
        vmem, anywhere = (pl.BlockSpec(memory_space=pltpu.VMEM), pl.BlockSpec(memory_space=pl.ANY))
        return pl.pallas_call(
            functools.partial(kernel, sp_size, tp_size),
            out_shape=jax.ShapeDtypeStruct((token_rows, width), bf16),
            in_specs=[vmem, pl.BlockSpec(memory_space=pltpu.SMEM)] + [vmem] * 3 + [anywhere] * 7,
            out_specs=vmem,
            scratch_shapes=[
                pltpu.VMEM((span, keys.shape[1]), bf16),
                pltpu.VMEM((span, keys.shape[1]), bf16),
                pltpu.VMEM((1, span), jnp.int32),
                pltpu.VMEM(w_out.shape, bf16),
                pltpu.VMEM((full, units), bf16),
                pltpu.VMEM((full, units), bf16),
                pltpu.VMEM((w_down.shape[1] * sp_size, units), bf16),
                pltpu.VMEM((rows, queries.shape[1]), bf16),
                pltpu.VMEM((tp_size, token_rows, queries.shape[1]), bf16),
                pltpu.VMEM((token_rows, width), f32),
                pltpu.VMEM((rows, width), bf16),
                pltpu.VMEM((rows, units), bf16),
                pltpu.VMEM(w_down.shape, bf16),
                pltpu.VMEM((tp_size, token_rows, width), bf16),
                pltpu.VMEM((others, token_rows, width), bf16),
                dma((7,)),
                dma((3, 2)),
                dma((3, 2)),
                dma((2, 4, chips // 2 + 1)),
                dma((2, 4, chips // 2 + 1)),
                dma((2, 4, chips // 2 + 1)),
                dma((2, 4, chips // 2 + 1)),
                dma((others,)),
                dma((others,)),
                dma((others,)),
                dma((others,)),
                dma((chips, others)),
                dma((chips, others)),
            ],
            compiler_params=pltpu.CompilerParams(
                collective_id=0, has_side_effects=True, vmem_limit_bytes=62 * 2**20
            ),
        )(
            queries,
            sink_logit,
            residual_in,
            gain_one[None, :],
            gain_two[None, :],
            keys,
            values,
            doc_ids[None, :],
            w_out,
            w_gate,
            w_up,
            w_down,
        )

    in_specs = (
        P("sp", "tp"),
        P("sp", "tp"),
        P("sp", "tp"),
        P("sp"),
        P("tp"),
        P(("sp", "tp"), None),
        P(),
        P(),
        P("sp", "tp"),
        P("sp", "tp"),
        P("tp", "sp"),
        P(),
    )
    return jax.shard_map(
        per_device, mesh=mesh, in_specs=in_specs, out_specs=P(("sp", "tp"), None), check_vma=False
    )
```
